32 devices in a mesh: grp: 2 (over y), sp: 4 (over z), tp: 4 (over x, core).
Axes of the slice: x: 2, y: 2, z: 4, core: 2. Of those that a mesh axis runs over, the one named last changes fastest.
Arguments:
- layer_input: bfloat16 [8, 1536, 2048], P(('grp', 'tp'), 'sp'), parts along dimension 0, may hold values from -6 to 6
- input_gain: float32 [2048], replicated, may hold values from 0.1 to 1.9
- key_weight: bfloat16 [2048, 512], replicated, may hold values from -0.125 to 0.125
- value_weight: bfloat16 [2048, 512], replicated, may hold values from -0.125 to 0.125
- stick_offsets: bfloat16 [4, 8, 1536], P(None, ('grp', 'tp'), 'sp'), parts along dimension 1
- head_bias: float32 [16], replicated
- queries: bfloat16 [8, 4, 512], P(('grp', 'tp'), 'sp'), parts along dimension 0, may hold values from -6 to 6
Outputs:
- key_cache: bfloat16 [8, 4, 1536, 128], P(('grp', 'tp'), 'sp'), parts along dimension 0
- value_cache: bfloat16 [8, 4, 1536, 128], P(('grp', 'tp'), 'sp'), parts along dimension 0
- offset_cache: bfloat16 [8, 4, 1536], P(('grp', 'tp'), 'sp'), parts along dimension 0
- first_read: bfloat16 [8, 4, 512], P(('grp', 'tp'), 'sp'), parts along dimension 0
The draws below stay inside these ranges and needn't reach their ends.
There are 2 independent parts, one for each index of `grp`. The reference program is written for one: setup_inputs(seed, part) draws one part's arguments, and reference() takes and returns one part's arrays. A program takes and returns all parts, laid end to end along the dimension named above; an argument that names none is the same for every part. Nothing has to cross between parts.
All inputs are finite; a program needn't handle non-finite values.
Results may differ from the reference program's by a relative error of at most 0.014.
Values may be sent and summed in bfloat16 or wider, within the bound.
A program may use at most 64 MiB of HBM per device.

```python
import math
import jax
import jax.numpy as jnp
from jax import lax

D = 2048
H = 16
KVH = 4
HD = 128
BLOCK = 384
QG = 4
SEQS = 4
LEN = 1536
N_SP = 4
N_TP = 4


def draw_head_bias(key, part):
    pick_key = jax.random.fold_in(key, 11)
    slow_key = jax.random.fold_in(key, 12)
    fast_key = jax.random.fold_in(key, 13)
    fast_share = 0.5
    fast_heads = jax.random.bernoulli(pick_key, fast_share, (H,))
    slow_value = -math.log(LEN) - jax.random.uniform(slow_key, (H,), jnp.float32, 0.5, 1.5)
    fast_value = -4.0 + jax.random.uniform(fast_key, (H,), jnp.float32, -0.5, 0.5)
    return jnp.where(fast_heads, fast_value, slow_value).astype(jnp.float32)


def draw_stick_offsets(key, part):
    level_key = jax.random.fold_in(key, 21)
    jitter_key = jax.random.fold_in(key, 22)
    place_key = jax.random.fold_in(key, 23)
    height_key = jax.random.fold_in(key, 24)
    level_range = 0.7
    blocks = LEN // BLOCK
    tier_entries = jax.random.uniform(level_key, (KVH, SEQS, blocks), jnp.float32, -level_range, level_range)
    tier_entries = jnp.repeat(tier_entries, BLOCK, axis=2)
    stochastic_jitter = jnp.clip(0.3 * jax.random.normal(jitter_key, (KVH, SEQS, LEN), jnp.float32), -1.0, 1.0)
    slot_destinations = jax.random.randint(place_key, (KVH, SEQS, 2), 0, LEN)
    vertical_extent_entries = math.log(LEN) + jax.random.uniform(height_key, (KVH, SEQS, 2), jnp.float32, 0.0, 1.0)
    sequence_slot_index = jnp.arange(LEN)
    clustered_sets = jnp.sum(jnp.where(sequence_slot_index[None, None, None, :] == slot_destinations[..., None], vertical_extent_entries[..., None], 0.0), axis=2)
    return (tier_entries + stochastic_jitter + clustered_sets).astype(jnp.bfloat16)


def level_of(stream_key, shape, cuts, least, top_value):
    def one(position, blocks):
        steps = jax.random.uniform(jax.random.fold_in(jax.random.fold_in(stream_key, 6), position), (blocks,), jnp.float32, least / len(cuts), top_value / len(cuts))
        return jnp.repeat(jnp.exp(steps), shape[position] // blocks).reshape((-1,) + (1,) * (len(shape) - position - 1))

    loudness = one(*cuts[0])
    for cut in cuts[1:]:
        loudness = loudness * one(*cut)
    return loudness


def normal_values(stream_key, dims, scale, bound, split=(), held_as=jnp.bfloat16):
    entries = jax.random.normal(stream_key, dims, jnp.float32) * scale
    if len(split) > 0:
        entries = level_of(stream_key, dims, split, -0.22, 0.18) * entries
    return jnp.clip(entries, min=-bound, max=bound).astype(held_as)


def setup_inputs(seed: int = 0, part: int = 0) -> dict:
    seeds = jax.random.split(jax.random.key(seed), 8)
    part_splits = jax.random.split(jax.random.fold_in(seeds[7], part), 8)
    return {
        "layer_input": normal_values(part_splits[0], (SEQS, LEN, D), 1.0, 6.0, ((0, 4), (1, 4))),
        "input_gain": jnp.clip(1.0 + 0.18 * jax.random.normal(seeds[1], (D,), jnp.float32), 0.1, 1.9),
        "key_weight": normal_values(seeds[2], (D, KVH * HD), D ** -0.5, 0.125),
        "value_weight": normal_values(seeds[3], (D, KVH * HD), D ** -0.5, 0.125),
        "stick_offsets": draw_stick_offsets(jax.random.fold_in(jax.random.fold_in(seeds[7], part), 71), part),
        "head_bias": draw_head_bias(jax.random.fold_in(seeds[7], 71), part),
        "queries": normal_values(part_splits[6], (N_TP, N_SP, QG * HD), 1.0, 6.0, ((0, 4), (1, 4))),
    }


EPSILON = 1e-06

def rms_scale(matrix):
    return matrix * lax.rsqrt(lax.optimization_barrier(jnp.mean(matrix * matrix, axis=-1, keepdims=True)) + EPSILON)

def stick_weights(scores, spread, carried):
    inside = lax.cumsum(spread, axis=scores.ndim - 1, reverse=True) - spread
    return jnp.exp(jax.nn.log_sigmoid(scores) - inside - carried)

def reference(layer_input, input_gain, key_weight, value_weight, stick_offsets, head_bias, queries):
    group_size = H // KVH
    per_column = N_SP // KVH

    def one_sequence(tokens):
        widened = tokens.astype(jnp.float32)
        normed_rows = (rms_scale(widened) * input_gain).astype(jnp.bfloat16)
        key_rows = jnp.dot(normed_rows, key_weight, preferred_element_type=jnp.float32).astype(jnp.bfloat16)
        value_rows = jnp.dot(normed_rows, value_weight, preferred_element_type=jnp.float32).astype(jnp.bfloat16)
        return (key_rows, value_rows)
    key_rows, value_rows = lax.map(one_sequence, layer_input)
    key_cache = jnp.transpose(key_rows.reshape(N_TP, per_column, LEN, KVH, HD), (0, 1, 3, 2, 4)).reshape(N_TP, N_SP, LEN, HD)
    value_cache = jnp.transpose(value_rows.reshape(N_TP, per_column, LEN, KVH, HD), (0, 1, 3, 2, 4)).reshape(N_TP, N_SP, LEN, HD)
    offset_cache = jnp.transpose(stick_offsets.reshape(KVH, N_TP, per_column, LEN), (1, 2, 0, 3)).reshape(N_TP, N_SP, LEN)
    bias_all = jnp.tile(head_bias.reshape(KVH, group_size), (N_TP * per_column, 1))

    def one_read(pieces):
        query_row, key_block, value_block, offset_row, bias_row = pieces
        scores = jnp.dot(query_row.reshape(group_size, HD), key_block.T, preferred_element_type=jnp.float32)
        scores = scores / math.sqrt(HD) + bias_row[:, None] + offset_row.astype(jnp.float32)[None, :]
        spread = jax.nn.softplus(scores)
        weights = stick_weights(scores, spread, 0.0).astype(jnp.bfloat16)
        mixture = jnp.dot(weights, value_block, preferred_element_type=jnp.float32)
        return rms_scale(mixture).astype(jnp.bfloat16).reshape(group_size * HD)
    first_read = lax.map(one_read, (queries.reshape(N_TP * N_SP, group_size * HD), key_cache.reshape(N_TP * N_SP, LEN, HD), value_cache.reshape(N_TP * N_SP, LEN, HD), offset_cache.reshape(N_TP * N_SP, LEN), bias_all))
    return (key_cache, value_cache, offset_cache, first_read.reshape(N_TP, N_SP, group_size * HD))
```

```python
import functools
import math

import jax
import jax.numpy as jnp
from jax import lax
from jax.experimental import pallas as pl
from jax.experimental.pallas import tpu as pltpu
from jax.sharding import PartitionSpec as P

H = 16
KVH = 4
HD = 128
EPSILON = 1e-06
ROWS = 128
VMEM_BYTES = 67043328
SPARE_BYTES = 262144
MESH = pl.DeviceIdType.MESH


def ring_order(count):
    return sorted(range(1, count), key=lambda d: (min(d, count - d), d))


def kernel(
    n, seqs, x_hbm, gain_ref, wk_hbm, wv_hbm, off_hbm, bias_ref, q_hbm,
    k_land, v_land, off_out, read_out,
    x_buf, normed, weights, sends, off_in, off_send, off_land, q_buf, stick,
    x_sem, w_sem, small_sem, k_sem, v_sem, o_sem,
):
    total, width = x_buf.shape
    block = total // seqs
    length = n * block
    group = H // KVH
    me = lax.axis_index("sp")
    order = ring_order(n)
    head_order = []
    for d in order + [0]:
        if d % KVH not in head_order:
            head_order.append(d % KVH)

    def peer(d):
        return lax.rem(me + d, n)

    def source(d):
        return lax.rem(me + n - d, n)

    x_copies = []
    for c in range(total // ROWS):
        part = pl.ds(c * ROWS, ROWS)
        x_copies.append(pltpu.make_async_copy(x_hbm.at[part], x_buf.at[part], x_sem.at[c]))
        x_copies[-1].start()
    w_copies = {}
    for kind, w_hbm in enumerate((wk_hbm, wv_hbm)):
        for j in head_order:
            col = pl.multiple_of(lax.rem(me + j, KVH) * HD, HD)
            copy = pltpu.make_async_copy(
                w_hbm.at[:, pl.ds(col, HD)], weights.at[kind, j], w_sem.at[kind, j]
            )
            copy.start()
            w_copies[kind, j] = copy
    off_copy = pltpu.make_async_copy(off_hbm, off_in, small_sem.at[0])
    off_copy.start()
    q_copy = pltpu.make_async_copy(q_hbm, q_buf, small_sem.at[1])
    q_copy.start()

    barrier = pltpu.get_barrier_semaphore()
    for d in order:
        pl.semaphore_signal(barrier, inc=1, device_id={"sp": peer(d)}, device_id_type=MESH)

    gain = gain_ref[...]
    step_rows = 16
    for c in range(total // ROWS):
        x_copies[c].wait()

        def norm_step(i, _, c=c):
            rows = pl.ds(pl.multiple_of(c * ROWS + i * step_rows, step_rows), step_rows)
            x = x_buf[rows, :].astype(jnp.float32)
            scale = lax.rsqrt(jnp.mean(x * x, axis=-1, keepdims=True) + EPSILON)
            normed[rows, :] = (x * scale * gain).astype(jnp.bfloat16)
            return 0

        lax.fori_loop(0, ROWS // step_rows, norm_step, 0, unroll=4)

    waited = set()

    def project(kind, d, dst):
        j = d % KVH
        if (kind, j) not in waited:
            w_copies[kind, j].wait()
            waited.add((kind, j))
        base = 0 if seqs == 1 else lax.div(peer(d), KVH) * block
        if seqs == 1:
            rows = normed[...]
        else:
            rows = normed[pl.ds(pl.multiple_of(base, 16), block), :]
        dst[...] = jnp.dot(rows, weights[kind, j], preferred_element_type=jnp.float32).astype(jnp.bfloat16)

    def send(src, dst, sem, slot, d):
        copy = pltpu.make_async_remote_copy(
            src_ref=src, dst_ref=dst, send_sem=sem.at[0, slot], recv_sem=sem.at[1, slot],
            device_id={"sp": peer(d)}, device_id_type=MESH,
        )
        copy.start()
        return copy

    here = pl.ds(pl.multiple_of(me * block, block), block)
    k_copies, v_copies, o_copies = {}, {}, {}
    for i, d in enumerate(order):
        project(0, d, sends.at[0, d])
        if i == 0:
            pl.semaphore_wait(barrier, n - 1)
        k_copies[d] = send(sends.at[0, d], k_land.at[0, 0, here], k_sem, d, d)
        if i == 0:
            off_copy.wait()
            for s in range(seqs):
                values = off_in[s].astype(jnp.float32)
                for h in range(KVH):
                    off_send[s * KVH + h] = values[h:h + 1, :]
            off_land[me] = off_send[me]
    for d in order:
        o_copies[d] = send(off_send.at[peer(d)], off_land.at[me], o_sem, d, d)
    project(0, 0, k_land.at[0, 0, here])
    for d in order:
        project(1, d, sends.at[1, d])
        v_copies[d] = send(sends.at[1, d], v_land.at[0, 0, here], v_sem, d, d)
    project(1, 0, v_land.at[0, 0, here])

    q_copy.wait()
    q_all = q_buf[0].astype(jnp.float32)
    q_rows = jnp.concatenate([q_all[:, g * HD:(g + 1) * HD] for g in range(group)] * 2, axis=0)
    q_rows = q_rows.astype(jnp.bfloat16)
    for d in order:
        o_copies[d].wait_recv()
    off_row = jnp.concatenate([off_land[i] for i in range(n)], axis=1)
    off_out[0] = off_row.astype(jnp.bfloat16)
    head = lax.rem(me, KVH)
    row_id = lax.broadcasted_iota(jnp.int32, (2 * group, 1), 0)
    bias = jnp.zeros((2 * group, 1), jnp.float32)
    for g in range(group):
        value = bias_ref[head * group + g]
        bias = jnp.where((row_id == g) | (row_id == g + group), value, bias)
    for d in order:
        k_copies[d].wait_recv()
    scores = lax.dot_general(
        q_rows, k_land[0, 0], (((1,), (1,)), ((), ())), preferred_element_type=jnp.float32
    )
    scores = scores / math.sqrt(HD) + bias + off_row
    tail = jnp.log1p(jnp.exp(-jnp.abs(scores)))
    spread = jnp.maximum(scores, 0.0) + tail
    log_sig = jnp.minimum(scores, 0.0) - tail
    chunks = length // HD
    cut = [spread[:, c * HD:(c + 1) * HD] for c in range(chunks)]
    stacked = jnp.concatenate(cut, axis=0)
    after = (
        lax.broadcasted_iota(jnp.int32, (HD, HD), 0) > lax.broadcasted_iota(jnp.int32, (HD, HD), 1)
    ).astype(jnp.float32)
    inner = jnp.dot(
        stacked, after, preferred_element_type=jnp.float32, precision=lax.Precision.HIGHEST
    )
    sums = jnp.sum(stacked, axis=1, keepdims=True)
    carried = jnp.zeros((2 * group, 1), jnp.float32)
    for c in reversed(range(chunks)):
        rows = slice(c * 2 * group, (c + 1) * 2 * group)
        beyond = inner[rows] + carried
        stick[:, c * HD:(c + 1) * HD] = jnp.exp(log_sig[:, c * HD:(c + 1) * HD] - beyond)
        carried = carried + sums[rows]

    mixture = jnp.zeros((2 * group, HD), jnp.float32)
    for d in [0] + order:
        if d:
            v_copies[d].wait_recv()
        part = pl.ds(pl.multiple_of(source(d) * block, block), block)
        mixture = mixture + jnp.dot(
            stick[:, part].astype(jnp.bfloat16), v_land[0, 0, part, :], preferred_element_type=jnp.float32
        )
    scale = lax.rsqrt(jnp.mean(mixture * mixture, axis=-1, keepdims=True) + EPSILON)
    read = mixture * scale
    read_out[0] = jnp.concatenate([read[g:g + 1] for g in range(group)], axis=1).astype(jnp.bfloat16)

    for d in order:
        k_copies[d].wait_send()
        v_copies[d].wait_send()
        o_copies[d].wait_send()


def shards(layer_input, input_gain, key_weight, value_weight, stick_offsets, head_bias, queries):
    seqs, block, width = layer_input.shape
    n = lax.axis_size("sp")
    length = n * block
    total = seqs * block
    hbm = pl.BlockSpec(memory_space=pltpu.HBM)
    vmem = pl.BlockSpec(memory_space=pltpu.VMEM)
    smem = pl.BlockSpec(memory_space=pltpu.SMEM)
    group_width = queries.shape[-1]
    return pl.pallas_call(
        functools.partial(kernel, n, seqs),
        out_shape=(
            jax.ShapeDtypeStruct((1, 1, length, HD), jnp.bfloat16),
            jax.ShapeDtypeStruct((1, 1, length, HD), jnp.bfloat16),
            jax.ShapeDtypeStruct((1, 1, length), jnp.bfloat16),
            jax.ShapeDtypeStruct((1, 1, group_width), jnp.bfloat16),
        ),
        in_specs=[hbm, vmem, hbm, hbm, hbm, smem, hbm],
        out_specs=(vmem, vmem, vmem, vmem),
        scratch_shapes=[
            pltpu.VMEM((total, width), jnp.bfloat16),
            pltpu.VMEM((total, width), jnp.bfloat16),
            pltpu.VMEM((2, KVH, width, HD), jnp.bfloat16),
            pltpu.VMEM((2, n, block, HD), jnp.bfloat16),
            pltpu.VMEM((seqs, KVH, block), jnp.bfloat16),
            pltpu.VMEM((n, 1, block), jnp.float32),
            pltpu.VMEM((n, 1, block), jnp.float32),
            pltpu.VMEM((1, 1, group_width), jnp.bfloat16),
            pltpu.VMEM((2 * (H // KVH), length), jnp.float32),
            pltpu.SemaphoreType.DMA((total // ROWS,)),
            pltpu.SemaphoreType.DMA((2, KVH)),
            pltpu.SemaphoreType.DMA((2,)),
            pltpu.SemaphoreType.DMA((2, n)),
            pltpu.SemaphoreType.DMA((2, n)),
            pltpu.SemaphoreType.DMA((2, n)),
        ],
        compiler_params=pltpu.CompilerParams(
            collective_id=0, has_side_effects=True, vmem_limit_bytes=VMEM_BYTES - 4 * length * HD - SPARE_BYTES
        ),
    )(
        layer_input.reshape(total, width),
        input_gain.reshape(1, width),
        key_weight,
        value_weight,
        jnp.transpose(stick_offsets, (1, 0, 2)),
        head_bias,
        queries,
    )


def solution(mesh):
    placed = (
        P(("grp", "tp"), "sp", None),
        P(),
        P(),
        P(),
        P(None, ("grp", "tp"), "sp"),
        P(),
        P(("grp", "tp"), "sp", None),
    )
    return jax.shard_map(
        shards,
        mesh=mesh,
        in_specs=placed,
        out_specs=(
            P(("grp", "tp"), "sp", None, None),
            P(("grp", "tp"), "sp", None, None),
            P(("grp", "tp"), "sp", None),
            P(("grp", "tp"), "sp", None),
        ),
        check_vma=False,
    )
```

```python
import functools
import math

import jax
import jax.numpy as jnp
from jax import lax
from jax.experimental import pallas as pl
from jax.experimental.pallas import tpu as pltpu
from jax.sharding import PartitionSpec as P

H = 16
KVH = 4
HD = 128
EPSILON = 1e-06
ROWS = 128
VMEM_BYTES = 67043328
SPARE_BYTES = 262144
WRITE_BYTES = 1048576
MESH = pl.DeviceIdType.MESH


def ring_order(count):
    return sorted(range(1, count), key=lambda d: (min(d, count - d), d))


def kernel(
    n, seqs, x_hbm, gain_ref, wk_hbm, wv_hbm, off_hbm, bias_ref, q_hbm,
    k_land, v_land, off_out, read_out,
    x_buf, normed, weights, sends, off_in, off_send, off_land, q_buf, stick,
    x_sem, w_sem, small_sem, k_sem, v_sem, o_sem,
):
    total, width = x_buf.shape
    block = total // seqs
    length = n * block
    group = H // KVH
    me = lax.axis_index("sp")
    order = ring_order(n)
    head_order = []
    for d in order + [0]:
        if d % KVH not in head_order:
            head_order.append(d % KVH)

    def peer(d):
        return lax.rem(me + d, n)

    def source(d):
        return lax.rem(me + n - d, n)

    x_copies = []
    for c in range(total // ROWS):
        part = pl.ds(c * ROWS, ROWS)
        x_copies.append(pltpu.make_async_copy(x_hbm.at[part], x_buf.at[part], x_sem.at[c]))
        x_copies[-1].start()
    w_copies = {}
    for kind, w_hbm in enumerate((wk_hbm, wv_hbm)):
        for j in head_order:
            col = pl.multiple_of(lax.rem(me + j, KVH) * HD, HD)
            copy = pltpu.make_async_copy(
                w_hbm.at[:, pl.ds(col, HD)], weights.at[kind, j], w_sem.at[kind, j]
            )
            copy.start()
            w_copies[kind, j] = copy
    off_copy = pltpu.make_async_copy(off_hbm, off_in, small_sem.at[0])
    off_copy.start()
    q_copy = pltpu.make_async_copy(q_hbm, q_buf, small_sem.at[1])
    q_copy.start()

    barrier = pltpu.get_barrier_semaphore()
    for d in order:
        pl.semaphore_signal(barrier, inc=1, device_id={"sp": peer(d)}, device_id_type=MESH)

    gain = gain_ref[...]
    step_rows = 16
    for c in range(total // ROWS):
        x_copies[c].wait()

        def norm_step(i, _, c=c):
            rows = pl.ds(pl.multiple_of(c * ROWS + i * step_rows, step_rows), step_rows)
            x = x_buf[rows, :].astype(jnp.float32)
            scale = lax.rsqrt(jnp.mean(x * x, axis=-1, keepdims=True) + EPSILON)
            normed[rows, :] = (x * scale * gain).astype(jnp.bfloat16)
            return 0

        lax.fori_loop(0, ROWS // step_rows, norm_step, 0, unroll=4)

    waited = set()

    def project(kind, d, dst):
        j = d % KVH
        if (kind, j) not in waited:
            w_copies[kind, j].wait()
            waited.add((kind, j))
        base = 0 if seqs == 1 else lax.div(peer(d), KVH) * block
        if seqs == 1:
            rows = normed[...]
        else:
            rows = normed[pl.ds(pl.multiple_of(base, 16), block), :]
        dst[...] = jnp.dot(rows, weights[kind, j], preferred_element_type=jnp.float32).astype(jnp.bfloat16)

    def send(src, dst, sem, slot, d):
        copy = pltpu.make_async_remote_copy(
            src_ref=src, dst_ref=dst, send_sem=sem.at[0, slot], recv_sem=sem.at[1, slot],
            device_id={"sp": peer(d)}, device_id_type=MESH,
        )
        copy.start()
        return copy

    here = pl.ds(pl.multiple_of(me * block, block), block)
    k_copies, v_copies, o_copies = {}, {}, {}
    for i, d in enumerate(order):
        project(0, d, sends.at[0, d])
        if i == 0:
            pl.semaphore_wait(barrier, n - 1)
        k_copies[d] = send(sends.at[0, d], k_land.at[0, 0, here], k_sem, d, d)
        if i == 0:
            off_copy.wait()
            for s in range(seqs):
                values = off_in[s].astype(jnp.float32)
                for h in range(KVH):
                    off_send[s * KVH + h] = values[h:h + 1, :]
            off_land[me] = off_send[me]
    for d in order:
        o_copies[d] = send(off_send.at[peer(d)], off_land.at[me], o_sem, d, d)
    project(0, 0, k_land.at[0, 0, here])
    for d in order:
        project(1, d, sends.at[1, d])
        v_copies[d] = send(sends.at[1, d], v_land.at[0, 0, here], v_sem, d, d)
    project(1, 0, v_land.at[0, 0, here])

    q_copy.wait()
    q_all = q_buf[0].astype(jnp.float32)
    q_rows = jnp.concatenate([q_all[:, g * HD:(g + 1) * HD] for g in range(group)] * 2, axis=0)
    q_rows = q_rows.astype(jnp.bfloat16)
    for d in order:
        o_copies[d].wait_recv()
    off_row = jnp.concatenate([off_land[i] for i in range(n)], axis=1)
    off_out[0] = off_row.astype(jnp.bfloat16)
    head = lax.rem(me, KVH)
    row_id = lax.broadcasted_iota(jnp.int32, (2 * group, 1), 0)
    bias = jnp.zeros((2 * group, 1), jnp.float32)
    for g in range(group):
        value = bias_ref[head * group + g]
        bias = jnp.where((row_id == g) | (row_id == g + group), value, bias)
    for d in order:
        k_copies[d].wait_recv()
    scores = lax.dot_general(
        q_rows, k_land[0, 0], (((1,), (1,)), ((), ())), preferred_element_type=jnp.float32
    )
    scores = scores / math.sqrt(HD) + bias + off_row
    tail = jnp.log1p(jnp.exp(-jnp.abs(scores)))
    spread = jnp.maximum(scores, 0.0) + tail
    log_sig = jnp.minimum(scores, 0.0) - tail
    chunks = length // HD
    cut = [spread[:, c * HD:(c + 1) * HD] for c in range(chunks)]
    stacked = jnp.concatenate(cut, axis=0)
    after = (
        lax.broadcasted_iota(jnp.int32, (HD, HD), 0) > lax.broadcasted_iota(jnp.int32, (HD, HD), 1)
    ).astype(jnp.float32)
    inner = jnp.dot(
        stacked, after, preferred_element_type=jnp.float32, precision=lax.Precision.HIGHEST
    )
    sums = jnp.sum(stacked, axis=1, keepdims=True)
    carried = jnp.zeros((2 * group, 1), jnp.float32)
    for c in reversed(range(chunks)):
        rows = slice(c * 2 * group, (c + 1) * 2 * group)
        beyond = inner[rows] + carried
        stick[:, c * HD:(c + 1) * HD] = jnp.exp(log_sig[:, c * HD:(c + 1) * HD] - beyond)
        carried = carried + sums[rows]

    mixture = jnp.zeros((2 * group, HD), jnp.float32)
    for d in [0] + order:
        if d:
            v_copies[d].wait_recv()
        part = pl.ds(pl.multiple_of(source(d) * block, block), block)
        mixture = mixture + jnp.dot(
            stick[:, part].astype(jnp.bfloat16), v_land[0, 0, part, :], preferred_element_type=jnp.float32
        )
    scale = lax.rsqrt(jnp.mean(mixture * mixture, axis=-1, keepdims=True) + EPSILON)
    read = mixture * scale
    read_out[0] = jnp.concatenate([read[g:g + 1] for g in range(group)], axis=1).astype(jnp.bfloat16)

    for d in order:
        k_copies[d].wait_send()
        v_copies[d].wait_send()
        o_copies[d].wait_send()


def write_out(*refs):
    *refs, sem = refs
    half = len(refs) // 2
    copies = [
        pltpu.make_async_copy(refs[i], refs[half + i], sem.at[i]) for i in range(half)
    ]
    for copy in copies:
        copy.start()
    for copy in copies:
        copy.wait()


def shards(layer_input, input_gain, key_weight, value_weight, stick_offsets, head_bias, queries):
    seqs, block, width = layer_input.shape
    n = lax.axis_size("sp")
    length = n * block
    total = seqs * block
    hbm = pl.BlockSpec(memory_space=pltpu.HBM)
    vmem = pl.BlockSpec(memory_space=pltpu.VMEM)
    smem = pl.BlockSpec(memory_space=pltpu.SMEM)
    group_width = queries.shape[-1]
    outs = (
        ((1, 1, length, HD), jnp.bfloat16),
        ((1, 1, length, HD), jnp.bfloat16),
        ((1, 1, length), jnp.bfloat16),
        ((1, 1, group_width), jnp.bfloat16),
    )
    held = pl.pallas_call(
        functools.partial(kernel, n, seqs),
        out_shape=tuple(pltpu.VMEM(*out) for out in outs),
        in_specs=[hbm, vmem, hbm, hbm, hbm, smem, hbm],
        out_specs=(vmem, vmem, vmem, vmem),
        scratch_shapes=[
            pltpu.VMEM((total, width), jnp.bfloat16),
            pltpu.VMEM((total, width), jnp.bfloat16),
            pltpu.VMEM((2, KVH, width, HD), jnp.bfloat16),
            pltpu.VMEM((2, n, block, HD), jnp.bfloat16),
            pltpu.VMEM((seqs, KVH, block), jnp.bfloat16),
            pltpu.VMEM((n, 1, block), jnp.float32),
            pltpu.VMEM((n, 1, block), jnp.float32),
            pltpu.VMEM((1, 1, group_width), jnp.bfloat16),
            pltpu.VMEM((2 * (H // KVH), length), jnp.float32),
            pltpu.SemaphoreType.DMA((total // ROWS,)),
            pltpu.SemaphoreType.DMA((2, KVH)),
            pltpu.SemaphoreType.DMA((2,)),
            pltpu.SemaphoreType.DMA((2, n)),
            pltpu.SemaphoreType.DMA((2, n)),
            pltpu.SemaphoreType.DMA((2, n)),
        ],
        compiler_params=pltpu.CompilerParams(
            collective_id=0, has_side_effects=True, vmem_limit_bytes=VMEM_BYTES - 4 * length * HD - SPARE_BYTES
        ),
    )(
        layer_input.reshape(total, width),
        input_gain.reshape(1, width),
        key_weight,
        value_weight,
        jnp.transpose(stick_offsets, (1, 0, 2)),
        head_bias,
        queries,
    )
    return pl.pallas_call(
        write_out,
        out_shape=tuple(jax.ShapeDtypeStruct(*out) for out in outs),
        in_specs=[vmem] * len(outs),
        out_specs=(hbm,) * len(outs),
        scratch_shapes=[pltpu.SemaphoreType.DMA((len(outs),))],
        compiler_params=pltpu.CompilerParams(vmem_limit_bytes=WRITE_BYTES),
    )(*held)


def solution(mesh):
    placed = (
        P(("grp", "tp"), "sp", None),
        P(),
        P(),
        P(),
        P(None, ("grp", "tp"), "sp"),
        P(),
        P(("grp", "tp"), "sp", None),
    )
    return jax.shard_map(
        shards,
        mesh=mesh,
        in_specs=placed,
        out_specs=(
            P(("grp", "tp"), "sp", None, None),
            P(("grp", "tp"), "sp", None, None),
            P(("grp", "tp"), "sp", None),
            P(("grp", "tp"), "sp", None),
        ),
        check_vma=False,
    )
```

```python
import functools
import math

import jax
import jax.numpy as jnp
from jax import lax
from jax.experimental import pallas as pl
from jax.experimental.pallas import tpu as pltpu
from jax.sharding import PartitionSpec as P

H = 16
KVH = 4
HD = 128
EPSILON = 1e-06
ROWS = 128
VMEM_BYTES = 67043328
SPARE_BYTES = 262144
WRITE_BYTES = 1048576
MESH = pl.DeviceIdType.MESH


def kernel(
    n, seqs, x_hbm, gain_ref, wk_hbm, wv_hbm, off_hbm, bias_ref, q_hbm,
    k_land, v_land, off_out, read_out,
    x_buf, normed, weights, sends, off_in, off_send, off_land, q_buf, stick,
    x_sem, w_sem, small_sem, k_sem, v_sem, o_sem,
):
    total, width = x_buf.shape
    block = total // seqs
    length = n * block
    group = H // KVH
    me = lax.axis_index("sp")
    order = range(1, n)
    paired = jnp.minimum(me, n - 1 - me)
    toward = jnp.where(2 * me < n, 1, -1)

    def peer(i):
        near = me + toward * (1 if i % 2 else -1) * ((i + 1) // 2)
        far = me + toward * (i - paired)
        return jnp.where(i <= 2 * paired, near, far) if i else me

    def offset(i):
        return lax.rem(peer(i) - me + n, n)

    def source(d):
        return lax.rem(me + n - d, n)

    first_head = lax.rem(peer(1), KVH)

    def slot(i):
        return lax.rem(lax.rem(peer(i), KVH) - first_head + KVH, KVH)

    x_copies = []
    for c in range(total // ROWS):
        part = pl.ds(c * ROWS, ROWS)
        x_copies.append(pltpu.make_async_copy(x_hbm.at[part], x_buf.at[part], x_sem.at[c]))
    w_copies = {}
    for kind, w_hbm in enumerate((wk_hbm, wv_hbm)):
        for j in range(KVH):
            col = pl.multiple_of(lax.rem(first_head + j, KVH) * HD, HD)
            w_copies[kind, j] = pltpu.make_async_copy(
                w_hbm.at[:, pl.ds(col, HD)], weights.at[kind, j], w_sem.at[kind, j]
            )
    x_copies[0].start()
    w_copies[0, 0].start()
    for copy in x_copies[1:]:
        copy.start()
    for key, copy in w_copies.items():
        if key != (0, 0):
            copy.start()
    off_copy = pltpu.make_async_copy(off_hbm, off_in, small_sem.at[0])
    off_copy.start()
    q_copy = pltpu.make_async_copy(q_hbm, q_buf, small_sem.at[1])
    q_copy.start()

    barrier = pltpu.get_barrier_semaphore()
    for d in order:
        pl.semaphore_signal(barrier, inc=1, device_id={"sp": source(d)}, device_id_type=MESH)

    gain = gain_ref[...]
    step_rows = 16
    for c in range(total // ROWS):
        x_copies[c].wait()

        def norm_step(i, _, c=c):
            rows = pl.ds(pl.multiple_of(c * ROWS + i * step_rows, step_rows), step_rows)
            x = x_buf[rows, :].astype(jnp.float32)
            scale = lax.rsqrt(jnp.mean(x * x, axis=-1, keepdims=True) + EPSILON)
            normed[rows, :] = (x * scale * gain).astype(jnp.bfloat16)
            return 0

        lax.fori_loop(0, ROWS // step_rows, norm_step, 0, unroll=4)

    def project(kind, i, dst):
        if i == 1:
            w_copies[kind, 0].wait()
        if i == 2:
            for j in range(1, KVH):
                w_copies[kind, j].wait()
        if seqs == 1:
            rows = normed[...]
        else:
            base = lax.div(peer(i), KVH) * block
            rows = normed[pl.ds(pl.multiple_of(base, 16), block), :]
        dst[...] = jnp.dot(
            rows, weights[kind, slot(i)], preferred_element_type=jnp.float32
        ).astype(jnp.bfloat16)

    def remote(src, dst, sem, d, target):
        return pltpu.make_async_remote_copy(
            src_ref=src, dst_ref=dst, send_sem=sem.at[0, d], recv_sem=sem.at[1, d],
            device_id={"sp": target}, device_id_type=MESH,
        )

    here = pl.ds(pl.multiple_of(me * block, block), block)

    def block_copy(kind, i):
        land, sem = ((k_land, k_sem), (v_land, v_sem))[kind]
        return remote(sends.at[kind, i], land.at[0, 0, here], sem, offset(i), peer(i))

    def offset_copy(i):
        return remote(off_send.at[peer(i)], off_land.at[me], o_sem, offset(i), peer(i))

    for i in order:
        project(0, i, sends.at[0, i])
        if i == 1:
            pl.semaphore_wait(barrier, n - 1)
        block_copy(0, i).start()
        if i == 1:
            off_copy.wait()
            for s in range(seqs):
                values = off_in[s].astype(jnp.float32)
                for h in range(KVH):
                    off_send[s * KVH + h] = values[h:h + 1, :]
            off_land[me] = off_send[me]
    for i in order:
        offset_copy(i).start()
    for i in order:
        project(1, i, sends.at[1, i])
        block_copy(1, i).start()
    project(0, 0, k_land.at[0, 0, here])
    project(1, 0, v_land.at[0, 0, here])

    def rows_of(i):
        return pl.ds(pl.multiple_of(peer(i) * block, block), block)

    def arrived(src, land, sem, i):
        d = lax.rem(me - peer(i) + n, n)
        remote(src, land.at[0, 0, rows_of(i)], sem, d, peer(i)).wait_recv()

    q_copy.wait()
    q_all = q_buf[0].astype(jnp.float32)
    q_rows = jnp.concatenate([q_all[:, g * HD:(g + 1) * HD] for g in range(group)] * 2, axis=0)
    q_rows = q_rows.astype(jnp.bfloat16)
    for d in order:
        remote(off_send.at[0], off_land.at[source(d)], o_sem, d, source(d)).wait_recv()
    off_row = jnp.concatenate([off_land[i] for i in range(n)], axis=1)
    off_out[0] = off_row.astype(jnp.bfloat16)
    head = lax.rem(me, KVH)
    row_id = lax.broadcasted_iota(jnp.int32, (2 * group, 1), 0)
    bias = jnp.zeros((2 * group, 1), jnp.float32)
    for g in range(group):
        value = bias_ref[head * group + g]
        bias = jnp.where((row_id == g) | (row_id == g + group), value, bias)
    for d in order:
        arrived(sends.at[0, d], k_land, k_sem, d)
    scores = lax.dot_general(
        q_rows, k_land[0, 0], (((1,), (1,)), ((), ())), preferred_element_type=jnp.float32
    )
    scores = scores / math.sqrt(HD) + bias + off_row
    tail = jnp.log1p(jnp.exp(-jnp.abs(scores)))
    spread = jnp.maximum(scores, 0.0) + tail
    log_sig = jnp.minimum(scores, 0.0) - tail
    chunks = length // HD
    cut = [spread[:, c * HD:(c + 1) * HD] for c in range(chunks)]
    stacked = jnp.concatenate(cut, axis=0)
    after = (
        lax.broadcasted_iota(jnp.int32, (HD, HD), 0) > lax.broadcasted_iota(jnp.int32, (HD, HD), 1)
    ).astype(jnp.float32)
    inner = jnp.dot(
        stacked, after, preferred_element_type=jnp.float32, precision=lax.Precision.HIGHEST
    )
    sums = jnp.sum(stacked, axis=1, keepdims=True)
    carried = jnp.zeros((2 * group, 1), jnp.float32)
    for c in reversed(range(chunks)):
        rows = slice(c * 2 * group, (c + 1) * 2 * group)
        beyond = inner[rows] + carried
        stick[:, c * HD:(c + 1) * HD] = jnp.exp(log_sig[:, c * HD:(c + 1) * HD] - beyond)
        carried = carried + sums[rows]

    mixture = jnp.zeros((2 * group, HD), jnp.float32)
    for d in range(n):
        if d:
            arrived(sends.at[1, d], v_land, v_sem, d)
        part = rows_of(d)
        mixture = mixture + jnp.dot(
            stick[:, part].astype(jnp.bfloat16), v_land[0, 0, part, :], preferred_element_type=jnp.float32
        )
    scale = lax.rsqrt(jnp.mean(mixture * mixture, axis=-1, keepdims=True) + EPSILON)
    read = mixture * scale
    read_out[0] = jnp.concatenate([read[g:g + 1] for g in range(group)], axis=1).astype(jnp.bfloat16)

    for i in order:
        block_copy(0, i).wait_send()
        block_copy(1, i).wait_send()
        offset_copy(i).wait_send()


def write_out(*refs):
    *refs, sem = refs
    half = len(refs) // 2
    copies = [
        pltpu.make_async_copy(refs[i], refs[half + i], sem.at[i]) for i in range(half)
    ]
    for copy in copies:
        copy.start()
    for copy in copies:
        copy.wait()


def shards(layer_input, input_gain, key_weight, value_weight, stick_offsets, head_bias, queries):
    seqs, block, width = layer_input.shape
    n = lax.axis_size("sp")
    length = n * block
    total = seqs * block
    hbm = pl.BlockSpec(memory_space=pltpu.HBM)
    vmem = pl.BlockSpec(memory_space=pltpu.VMEM)
    smem = pl.BlockSpec(memory_space=pltpu.SMEM)
    group_width = queries.shape[-1]
    outs = (
        ((1, 1, length, HD), jnp.bfloat16),
        ((1, 1, length, HD), jnp.bfloat16),
        ((1, 1, length), jnp.bfloat16),
        ((1, 1, group_width), jnp.bfloat16),
    )
    held = pl.pallas_call(
        functools.partial(kernel, n, seqs),
        out_shape=tuple(pltpu.VMEM(*out) for out in outs),
        in_specs=[hbm, vmem, hbm, hbm, hbm, smem, hbm],
        out_specs=(vmem, vmem, vmem, vmem),
        scratch_shapes=[
            pltpu.VMEM((total, width), jnp.bfloat16),
            pltpu.VMEM((total, width), jnp.bfloat16),
            pltpu.VMEM((2, KVH, width, HD), jnp.bfloat16),
            pltpu.VMEM((2, n, block, HD), jnp.bfloat16),
            pltpu.VMEM((seqs, KVH, block), jnp.bfloat16),
            pltpu.VMEM((n, 1, block), jnp.float32),
            pltpu.VMEM((n, 1, block), jnp.float32),
            pltpu.VMEM((1, 1, group_width), jnp.bfloat16),
            pltpu.VMEM((2 * (H // KVH), length), jnp.float32),
            pltpu.SemaphoreType.DMA((total // ROWS,)),
            pltpu.SemaphoreType.DMA((2, KVH)),
            pltpu.SemaphoreType.DMA((2,)),
            pltpu.SemaphoreType.DMA((2, n)),
            pltpu.SemaphoreType.DMA((2, n)),
            pltpu.SemaphoreType.DMA((2, n)),
        ],
        compiler_params=pltpu.CompilerParams(
            collective_id=0, has_side_effects=True, vmem_limit_bytes=VMEM_BYTES - 4 * length * HD - SPARE_BYTES
        ),
    )(
        layer_input.reshape(total, width),
        input_gain.reshape(1, width),
        key_weight,
        value_weight,
        jnp.transpose(stick_offsets, (1, 0, 2)),
        head_bias,
        queries,
    )
    return pl.pallas_call(
        write_out,
        out_shape=tuple(jax.ShapeDtypeStruct(*out) for out in outs),
        in_specs=[vmem] * len(outs),
        out_specs=(hbm,) * len(outs),
        scratch_shapes=[pltpu.SemaphoreType.DMA((len(outs),))],
        compiler_params=pltpu.CompilerParams(vmem_limit_bytes=WRITE_BYTES),
    )(*held)


def solution(mesh):
    placed = (
        P(("grp", "tp"), "sp", None),
        P(),
        P(),
        P(),
        P(None, ("grp", "tp"), "sp"),
        P(),
        P(("grp", "tp"), "sp", None),
    )
    return jax.shard_map(
        shards,
        mesh=mesh,
        in_specs=placed,
        out_specs=(
            P(("grp", "tp"), "sp", None, None),
            P(("grp", "tp"), "sp", None, None),
            P(("grp", "tp"), "sp", None),
            P(("grp", "tp"), "sp", None),
        ),
        check_vma=False,
    )
```

```python
import functools
import math

import jax
import jax.numpy as jnp
from jax import lax
from jax.experimental import pallas as pl
from jax.experimental.pallas import tpu as pltpu
from jax.sharding import PartitionSpec as P

H = 16
KVH = 4
HD = 128
EPSILON = 1e-06
ROWS = 128
PIECES = 4
VMEM_BYTES = 67043328
SPARE_BYTES = 262144
WRITE_BYTES = 1048576
MESH = pl.DeviceIdType.MESH


def kernel(
    n, seqs, x_hbm, gain_ref, wk_hbm, wv_hbm, off_hbm, bias_ref, q_hbm,
    k_land, v_land, off_out, read_out,
    x_buf, normed, weights, sends, off_in, off_send, off_land, q_buf, stick,
    x_sem, w_sem, small_sem, k_sem, v_sem, o_sem,
):
    total, width = x_buf.shape
    block = total // seqs
    length = n * block
    group = H // KVH
    me = lax.axis_index("sp")
    order = range(1, n)
    paired = jnp.minimum(me, n - 1 - me)
    toward = jnp.where(2 * me < n, 1, -1)

    def peer(i):
        near = me + toward * (1 if i % 2 else -1) * ((i + 1) // 2)
        far = me + toward * (i - paired)
        return jnp.where(i <= 2 * paired, near, far) if i else me

    def offset(i):
        return lax.rem(peer(i) - me + n, n)

    def source(d):
        return lax.rem(me + n - d, n)

    def columns(i):
        return pl.ds(pl.multiple_of(lax.rem(peer(i), KVH) * HD, HD), HD)

    x_copies = []
    for c in range(total // ROWS):
        part = pl.ds(c * ROWS, ROWS)
        x_copies.append(pltpu.make_async_copy(x_hbm.at[part], x_buf.at[part], x_sem.at[c]))
    w_copies = {}
    for kind, w_hbm in enumerate((wk_hbm, wv_hbm)):
        for j in range(PIECES):
            part = pl.ds(j * (width // PIECES), width // PIECES)
            w_copies[kind, j] = pltpu.make_async_copy(
                w_hbm.at[part], weights.at[kind, part], w_sem.at[kind, j]
            )
    x_copies[0].start()
    for j in range(PIECES):
        w_copies[0, j].start()
    for copy in x_copies[1:]:
        copy.start()
    for j in range(PIECES):
        w_copies[1, j].start()
    off_copy = pltpu.make_async_copy(off_hbm, off_in, small_sem.at[0])
    off_copy.start()
    q_copy = pltpu.make_async_copy(q_hbm, q_buf, small_sem.at[1])
    q_copy.start()

    barrier = pltpu.get_barrier_semaphore()
    for d in order:
        pl.semaphore_signal(barrier, inc=1, device_id={"sp": source(d)}, device_id_type=MESH)

    gain = gain_ref[...]
    step_rows = 16
    def norm(c):
        x_copies[c].wait()

        def norm_step(i, _):
            rows = pl.ds(pl.multiple_of(c * ROWS + i * step_rows, step_rows), step_rows)
            x = x_buf[rows, :].astype(jnp.float32)
            scale = lax.rsqrt(jnp.mean(x * x, axis=-1, keepdims=True) + EPSILON)
            normed[rows, :] = (x * scale * gain).astype(jnp.bfloat16)
            return 0

        lax.fori_loop(0, ROWS // step_rows, norm_step, 0, unroll=4)

    def wait_weights(kind):
        for j in range(PIECES):
            w_copies[kind, j].wait()

    def project(kind, i, dst):
        if i == 1:
            wait_weights(kind)
        if seqs == 1:
            rows = normed[...]
        else:
            base = lax.div(peer(i), KVH) * block
            rows = normed[pl.ds(pl.multiple_of(base, 16), block), :]
        dst[...] = jnp.dot(
            rows, weights[kind, :, columns(i)], preferred_element_type=jnp.float32
        ).astype(jnp.bfloat16)

    def remote(src, dst, sem, d, target):
        return pltpu.make_async_remote_copy(
            src_ref=src, dst_ref=dst, send_sem=sem.at[0, d], recv_sem=sem.at[1, d],
            device_id={"sp": target}, device_id_type=MESH,
        )

    here = pl.ds(pl.multiple_of(me * block, block), block)

    def block_copy(kind, i):
        land, sem = ((k_land, k_sem), (v_land, v_sem))[kind]
        return remote(sends.at[kind, i], land.at[0, 0, here], sem, offset(i), peer(i))

    def offset_copy(i):
        return remote(off_send.at[peer(i)], off_land.at[me], o_sem, offset(i), peer(i))

    if seqs == 1:
        for c in range(total // ROWS):
            norm(c)
            if c == 0:
                wait_weights(0)
            part = pl.ds(c * ROWS, ROWS)
            sends[0, 1, part] = jnp.dot(
                normed[part, :], weights[0, :, columns(1)], preferred_element_type=jnp.float32
            ).astype(jnp.bfloat16)
            if c == 0:
                pl.semaphore_wait(barrier, n - 1)
            there = pl.ds(pl.multiple_of(me * block + c * ROWS, ROWS), ROWS)
            remote(
                sends.at[0, 1, part], k_land.at[0, 0, there], k_sem, offset(1), peer(1)
            ).start()
    else:
        for c in range(total // ROWS):
            norm(c)
    for i in order:
        if seqs > 1 or i > 1:
            project(0, i, sends.at[0, i])
            if i == 1:
                pl.semaphore_wait(barrier, n - 1)
            block_copy(0, i).start()
        if i == 1:
            off_copy.wait()
            for s in range(seqs):
                values = off_in[s].astype(jnp.float32)
                for h in range(KVH):
                    off_send[s * KVH + h] = values[h:h + 1, :]
            off_land[me] = off_send[me]
    for i in order:
        offset_copy(i).start()
    for i in order:
        project(1, i, sends.at[1, i])
        block_copy(1, i).start()
    project(0, 0, k_land.at[0, 0, here])
    project(1, 0, v_land.at[0, 0, here])

    def rows_of(i):
        return pl.ds(pl.multiple_of(peer(i) * block, block), block)

    def arrived(src, land, sem, i):
        d = lax.rem(me - peer(i) + n, n)
        remote(src, land.at[0, 0, rows_of(i)], sem, d, peer(i)).wait_recv()

    q_copy.wait()
    q_all = q_buf[0].astype(jnp.float32)
    q_rows = jnp.concatenate([q_all[:, g * HD:(g + 1) * HD] for g in range(group)] * 2, axis=0)
    q_rows = q_rows.astype(jnp.bfloat16)
    for d in order:
        remote(off_send.at[0], off_land.at[source(d)], o_sem, d, source(d)).wait_recv()
    off_row = jnp.concatenate([off_land[i] for i in range(n)], axis=1)
    off_out[0] = off_row.astype(jnp.bfloat16)
    head = lax.rem(me, KVH)
    row_id = lax.broadcasted_iota(jnp.int32, (2 * group, 1), 0)
    bias = jnp.zeros((2 * group, 1), jnp.float32)
    for g in range(group):
        value = bias_ref[head * group + g]
        bias = jnp.where((row_id == g) | (row_id == g + group), value, bias)
    for d in order:
        arrived(sends.at[0, d], k_land, k_sem, d)
    scores = lax.dot_general(
        q_rows, k_land[0, 0], (((1,), (1,)), ((), ())), preferred_element_type=jnp.float32
    )
    scores = scores / math.sqrt(HD) + bias + off_row
    tail = jnp.log1p(jnp.exp(-jnp.abs(scores)))
    spread = jnp.maximum(scores, 0.0) + tail
    log_sig = jnp.minimum(scores, 0.0) - tail
    chunks = length // HD
    cut = [spread[:, c * HD:(c + 1) * HD] for c in range(chunks)]
    stacked = jnp.concatenate(cut, axis=0)
    after = (
        lax.broadcasted_iota(jnp.int32, (HD, HD), 0) > lax.broadcasted_iota(jnp.int32, (HD, HD), 1)
    ).astype(jnp.float32)
    inner = jnp.dot(
        stacked, after, preferred_element_type=jnp.float32, precision=lax.Precision.HIGHEST
    )
    sums = jnp.sum(stacked, axis=1, keepdims=True)
    carried = jnp.zeros((2 * group, 1), jnp.float32)
    for c in reversed(range(chunks)):
        rows = slice(c * 2 * group, (c + 1) * 2 * group)
        beyond = inner[rows] + carried
        stick[:, c * HD:(c + 1) * HD] = jnp.exp(log_sig[:, c * HD:(c + 1) * HD] - beyond)
        carried = carried + sums[rows]

    mixture = jnp.zeros((2 * group, HD), jnp.float32)
    for d in range(n):
        if d:
            arrived(sends.at[1, d], v_land, v_sem, d)
        part = rows_of(d)
        mixture = mixture + jnp.dot(
            stick[:, part].astype(jnp.bfloat16), v_land[0, 0, part, :], preferred_element_type=jnp.float32
        )
    scale = lax.rsqrt(jnp.mean(mixture * mixture, axis=-1, keepdims=True) + EPSILON)
    read = mixture * scale
    read_out[0] = jnp.concatenate([read[g:g + 1] for g in range(group)], axis=1).astype(jnp.bfloat16)

    for i in order:
        block_copy(0, i).wait_send()
        block_copy(1, i).wait_send()
        offset_copy(i).wait_send()


def write_out(*refs):
    *refs, sem = refs
    half = len(refs) // 2
    copies = [
        pltpu.make_async_copy(refs[i], refs[half + i], sem.at[i]) for i in range(half)
    ]
    for copy in copies:
        copy.start()
    for copy in copies:
        copy.wait()


def shards(layer_input, input_gain, key_weight, value_weight, stick_offsets, head_bias, queries):
    seqs, block, width = layer_input.shape
    n = lax.axis_size("sp")
    length = n * block
    total = seqs * block
    hbm = pl.BlockSpec(memory_space=pltpu.HBM)
    vmem = pl.BlockSpec(memory_space=pltpu.VMEM)
    smem = pl.BlockSpec(memory_space=pltpu.SMEM)
    group_width = queries.shape[-1]
    outs = (
        ((1, 1, length, HD), jnp.bfloat16),
        ((1, 1, length, HD), jnp.bfloat16),
        ((1, 1, length), jnp.bfloat16),
        ((1, 1, group_width), jnp.bfloat16),
    )
    held = pl.pallas_call(
        functools.partial(kernel, n, seqs),
        out_shape=tuple(pltpu.VMEM(*out) for out in outs),
        in_specs=[hbm, vmem, hbm, hbm, hbm, smem, hbm],
        out_specs=(vmem, vmem, vmem, vmem),
        scratch_shapes=[
            pltpu.VMEM((total, width), jnp.bfloat16),
            pltpu.VMEM((total, width), jnp.bfloat16),
            pltpu.VMEM((2, width, KVH * HD), jnp.bfloat16),
            pltpu.VMEM((2, n, block, HD), jnp.bfloat16),
            pltpu.VMEM((seqs, KVH, block), jnp.bfloat16),
            pltpu.VMEM((n, 1, block), jnp.float32),
            pltpu.VMEM((n, 1, block), jnp.float32),
            pltpu.VMEM((1, 1, group_width), jnp.bfloat16),
            pltpu.VMEM((2 * (H // KVH), length), jnp.float32),
            pltpu.SemaphoreType.DMA((total // ROWS,)),
            pltpu.SemaphoreType.DMA((2, PIECES)),
            pltpu.SemaphoreType.DMA((2,)),
            pltpu.SemaphoreType.DMA((2, n)),
            pltpu.SemaphoreType.DMA((2, n)),
            pltpu.SemaphoreType.DMA((2, n)),
        ],
        compiler_params=pltpu.CompilerParams(
            collective_id=0, has_side_effects=True, vmem_limit_bytes=VMEM_BYTES - 4 * length * HD - SPARE_BYTES
        ),
    )(
        layer_input.reshape(total, width),
        input_gain.reshape(1, width),
        key_weight,
        value_weight,
        jnp.transpose(stick_offsets, (1, 0, 2)),
        head_bias,
        queries,
    )
    return pl.pallas_call(
        write_out,
        out_shape=tuple(jax.ShapeDtypeStruct(*out) for out in outs),
        in_specs=[vmem] * len(outs),
        out_specs=(hbm,) * len(outs),
        scratch_shapes=[pltpu.SemaphoreType.DMA((len(outs),))],
        compiler_params=pltpu.CompilerParams(vmem_limit_bytes=WRITE_BYTES),
    )(*held)


def solution(mesh):
    placed = (
        P(("grp", "tp"), "sp", None),
        P(),
        P(),
        P(),
        P(None, ("grp", "tp"), "sp"),
        P(),
        P(("grp", "tp"), "sp", None),
    )
    return jax.shard_map(
        shards,
        mesh=mesh,
        in_specs=placed,
        out_specs=(
            P(("grp", "tp"), "sp", None, None),
            P(("grp", "tp"), "sp", None, None),
            P(("grp", "tp"), "sp", None),
            P(("grp", "tp"), "sp", None),
        ),
        check_vma=False,
    )
```
